256 devices in a mesh: fs: 32 (over z, x), tp: 8 (over y, core).
Axes of the slice: x: 4, y: 4, z: 8, core: 2. Of those that a mesh axis runs over, the one named last changes fastest.
Arguments:
- tokens: bfloat16 [8192, 2048], P('fs', 'tp'), may hold values from -6 to 6
- grad_out: bfloat16 [8192, 2048], P('fs', 'tp'), may hold values from -6 to 6
- up_weight: bfloat16 [2048, 4096], P('fs', 'tp'), may hold values from -0.125 to 0.125
- down_weight: bfloat16 [4096, 2048], P('tp', 'fs'), may hold values from -0.09375 to 0.09375
Outputs:
- input_grad: bfloat16 [8192, 2048], P('fs', 'tp')
- up_grad: float32 [2048, 4096], P('fs', 'tp')
- down_grad: float32 [4096, 2048], P('tp', 'fs')
- up_norms: float32 [2048], P('fs')
- down_norms: float32 [4096], P('tp')
The draws below stay inside these ranges and needn't reach their ends.
All inputs are finite; a program needn't handle non-finite values.
Results may differ from the reference program's by a relative error of at most 0.015.
Values may be sent and summed in bfloat16 or wider, within the bound.
No kernel may reach another device: no remote copies, remote signals or barrier semaphores. Data moves between devices by JAX's collectives and lax.ppermute only.
A program may use at most 64 MiB of HBM per device.

```python
import jax
import jax.numpy as jnp

D = 2048
FF = 4096
TOKENS = 8192
N_TP = 8


def with_spikes(entries, own_key, source, target, blocks, factor):
    owner, partner = [(jnp.arange(entries.shape[dim]) // (entries.shape[dim] // blocks)).reshape([-1 if axis == dim else 1 for axis in range(entries.ndim)]) for dim in (source, target)]
    chosen = jax.random.permutation(own_key, blocks)[partner]
    strong = (owner == chosen) | (owner == (partner + blocks // 2) % blocks)
    return jnp.where(strong, factor * entries, entries)


def steps_of(key, shape, cuts, low, largest):
    gain = 1.0
    for axis_at, parts in cuts:
        steps = jax.random.uniform(jax.random.fold_in(jax.random.fold_in(key, 6), axis_at), (parts,), jnp.float32, low / len(cuts), largest / len(cuts))
        gain = gain * jnp.repeat(jnp.exp(steps), shape[axis_at] // parts).reshape((-1,) + (1,) * (len(shape) - 1 - axis_at))
    return gain


def centred(rng, shape, spread, bound, split=(), kind=jnp.bfloat16):
    entries = jax.random.normal(rng, shape, jnp.float32) * spread
    if len(split) > 0:
        entries = steps_of(rng, shape, split, -0.22, 0.18) * entries
    return jnp.clip(entries, min=-bound, max=bound).astype(kind)


def heavy_noise(stream_key, dims, spread, reach, shards, heavy, held_as=jnp.bfloat16):
    entries = spread * jax.random.normal(stream_key, dims, jnp.float32)
    if shards:
        entries = entries * steps_of(stream_key, dims, shards, -0.22, 0.18)
    return jnp.clip(with_spikes(entries, jax.random.fold_in(stream_key, 3), *heavy), -reach, reach).astype(held_as)


def setup_inputs(seed: int = 0) -> dict:
    splits = jax.random.split(jax.random.key(seed), 5)
    tokens = heavy_noise(splits[0], (TOKENS, D), 1.0, 6.0, ((0, 32), (1, 8)), (0, 1, 32, 2.75))
    grad_out = heavy_noise(splits[1], (TOKENS, D), 1.0, 6.0, ((0, 32), (1, 8)), (0, 1, 32, 2.75))
    up_weight = centred(splits[2], (D, FF), D ** -0.5, 0.125, ((0, 32), (1, 8)))
    down_weight = centred(splits[3], (FF, D), FF ** -0.5, 0.09375, ((0, 8), (1, 32)))
    return dict(tokens=tokens, grad_out=grad_out, up_weight=up_weight, down_weight=down_weight)


def reference(tokens, grad_out, up_weight, down_weight):
    pre = jnp.dot(tokens, up_weight, preferred_element_type=jnp.float32)
    relued = jnp.maximum(pre, 0.0)
    act = (relued * relued).astype(jnp.bfloat16)
    dact = jnp.dot(grad_out, down_weight.T, preferred_element_type=jnp.float32)
    dpre = (dact * 2.0 * relued).astype(jnp.bfloat16)
    down_grad = jnp.dot(act.T, grad_out, preferred_element_type=jnp.float32)
    up_grad = jnp.dot(tokens.T, dpre, preferred_element_type=jnp.float32)
    block = FF // N_TP
    total = jnp.zeros((tokens.shape[0], D), jnp.float32)
    for index in range(N_TP):
        part = jnp.dot(dpre[:, index * block:(index + 1) * block], up_weight[:, index * block:(index + 1) * block].T, preferred_element_type=jnp.float32)
        total = total + part.astype(jnp.bfloat16).astype(jnp.float32)
    input_grad = total.astype(jnp.bfloat16)
    up_norms = jnp.sum(up_grad * up_grad, axis=1)
    down_norms = jnp.sum(down_grad * down_grad, axis=1)
    return input_grad, up_grad, down_grad, up_norms, down_norms
```

```python
import jax
import jax.numpy as jnp
from jax import lax
from jax.sharding import Mesh
from jax.sharding import PartitionSpec as P


F32 = jnp.float32
BF16 = jnp.bfloat16


def exchange(parts, axes):
    return lax.all_to_all(parts, axes, split_axis=0, concat_axis=0, tiled=True)


def shift(x, axis, by):
    n = lax.axis_size(axis)
    return lax.ppermute(x, axis, [(i, (i + by) % n) for i in range(n)])


def ring_of_four(x, axis, dim):
    n, me = lax.axis_size(axis), lax.axis_index(axis)
    size = x.shape[dim]
    half = x.shape[0] // 2
    shape = list(x.shape)
    shape[dim] *= n
    out = jnp.zeros(shape, x.dtype)

    def put(out, block, offset, row=0):
        at = [0] * x.ndim
        at[0] = row
        at[dim] = at[dim] + lax.rem(me + offset + n, n) * size
        return lax.dynamic_update_slice(out, block, at)

    before, after = shift(x, axis, 1), shift(x, axis, -1)
    far_low = shift(before[:half], axis, 1)
    far_high = shift(after[half:], axis, -1)
    out = put(out, x, 0)
    out = put(out, before, -1)
    out = put(out, after, 1)
    out = put(out, far_low, 2)
    return put(out, far_high, 2, half)


def dot(a, b, ca, cb):
    return lax.dot_general(a, b, (((ca,), (cb,)), ((), ())), preferred_element_type=F32)


def on_device(tokens, grad_out, up_weight, down_weight):
    rows, feats = tokens.shape
    nx, ny, nz = (lax.axis_size(a) for a in ("x", "y", "z"))
    half = rows // 2
    d_rows, hid = up_weight.shape
    part = hid // nx
    d_model = d_rows * nz * nx

    w = jnp.stack([up_weight, down_weight.T]).reshape(2, d_rows, nx, part)
    w = exchange(w.transpose(2, 0, 1, 3), "x")
    w = exchange(jnp.broadcast_to(w, (nz, *w.shape)), "z")
    w_other = shift(w, "c", 1)
    weights = jnp.concatenate(
        [v.transpose(2, 0, 1, 3, 4).reshape(2, d_model, part) for v in (w, w_other)], axis=2
    )
    up, down = weights[0], weights[1]

    def halves(a, axis):
        n = lax.axis_size(axis)
        sent = jnp.broadcast_to(a.reshape(2, half, feats), (n, 2, half, feats))
        got = exchange(sent.reshape(n * 2, half, feats), (axis, "c"))
        return got.reshape(n, 2, half, feats).transpose(0, 2, 1, 3).reshape(n, half, 2 * feats)

    tok = halves(tokens, "x").reshape(nx * half, 2 * feats)
    tok = ring_of_four(tok, "y", 1)
    cot = halves(grad_out, "y").transpose(1, 0, 2).reshape(half, ny * 2 * feats)
    cot = ring_of_four(cot, "x", 0)

    pre = dot(tok, up, 1, 0)
    relued = jnp.maximum(pre, 0.0)
    act = (relued * relued).astype(BF16)
    dpre = (dot(cot, down, 1, 0) * 2.0 * relued).astype(BF16)

    up_part = dot(tok, dpre, 0, 0)
    down_part = dot(cot, act, 0, 0)
    kept = jnp.stack([up_part[:, :part], down_part[:, :part]]).astype(BF16)
    given = jnp.stack([up_part[:, part:], down_part[:, part:]]).astype(BF16)
    both = (kept.astype(F32) + shift(given, "c", 1).astype(F32)).astype(BF16)
    both = both.reshape(2, nz * nx, d_rows, part).transpose(1, 0, 2, 3)
    summed = exchange(both, ("z", "x")).reshape(nz, nx, 2, d_rows, part).astype(F32).sum(axis=0)
    grads = summed.transpose(1, 2, 0, 3).reshape(2, d_rows, hid)
    up_grad, down_flip = grads[0], grads[1]

    back = dot(dpre, up, 1, 1).astype(BF16)
    back = back.reshape(nx, half, ny, 2, feats).transpose(0, 2, 3, 1, 4)
    back = exchange(back.reshape(nx * ny * 2, half, feats), ("x", "y", "c"))
    input_grad = back.reshape(nx * ny, rows, feats).astype(F32).sum(axis=0).astype(BF16)

    def total(v, axes, n):
        sent = jnp.broadcast_to(v, (n, 1, *v.shape))
        return exchange(sent, axes).sum(axis=(0, 1))

    up_norms = total(jnp.sum(up_grad * up_grad, axis=1), ("y", "c"), ny * 2)
    down_norms = total(jnp.sum(down_flip * down_flip, axis=0), ("z", "x"), nz * nx)
    return input_grad, up_grad, down_flip.T, up_norms, down_norms


def solution(mesh):
    finer = Mesh(mesh.devices.reshape(8, 4, 4, 2), ("z", "x", "y", "c"))
    fs, tp = ("z", "x"), ("y", "c")
    return jax.shard_map(
        on_device,
        mesh=finer,
        in_specs=(P(fs, tp), P(fs, tp), P(fs, tp), P(tp, fs)),
        out_specs=(P(fs, tp), P(fs, tp), P(tp, fs), P(fs), P(tp)),
        check_vma=False,
    )
```

```python
import jax
import jax.numpy as jnp
from jax import lax
from jax.experimental import pallas as pl
from jax.experimental.pallas import tpu as pltpu
from jax.sharding import Mesh
from jax.sharding import PartitionSpec as P


F32 = jnp.float32
BF16 = jnp.bfloat16
N = 4
VMEM = pl.BlockSpec(memory_space=pltpu.VMEM)


def exchange(parts, axes):
    return lax.all_to_all(parts, axes, split_axis=0, concat_axis=0, tiled=True)


def shift(x, axis, by):
    n = lax.axis_size(axis)
    return lax.ppermute(x, axis, [(i, (i + by) % n) for i in range(n)])


def kernel(body, outs, args, flops, name):
    moved = sum(a.size * a.dtype.itemsize for a in args)
    return pl.pallas_call(
        body,
        out_shape=outs,
        in_specs=[VMEM] * len(args),
        out_specs=[VMEM] * len(outs),
        cost_estimate=pl.CostEstimate(flops=flops, bytes_accessed=moved, transcendentals=0),
        compiler_params=pltpu.CompilerParams(vmem_limit_bytes=48 * 2**20),
        name=name,
    )(*args)


def out(dtype, *dims):
    return jax.ShapeDtypeStruct(dims, dtype)


def dot(a, b, ca, cb):
    return lax.dot_general(a, b, (((ca,), (cb,)), ((), ())), preferred_element_type=F32)


def token_block(refs, ky, rc, kx):
    here, after, before, far_low, far_high = refs
    if ky == 0:
        return here[kx, rc]
    if ky == 1:
        return after[(kx + 2) % N, rc]
    if ky == 3:
        return before[kx, rc]
    return far_low[kx, rc] if kx < 2 else far_high[kx - 2, rc]


def cotan_block(refs, ky, rc, kx):
    here, after, before, far_low, far_high = refs
    if kx == 0:
        return here[ky, rc]
    if kx == 1:
        return after[(ky + 2) % N, rc]
    if kx == 3:
        return before[ky, rc]
    return far_low[ky, rc] if ky < 2 else far_high[ky - 2, rc]


def rows_of(block, refs, ky, rc):
    return jnp.concatenate([block(refs, ky, rc, kx) for kx in range(N)], axis=0)


def feature_block(ky, rc):
    y, c = lax.axis_index("y"), lax.axis_index("c")
    return 2 * lax.rem(y + ky, N) + (c if rc == 0 else 1 - c)


def weight_block(mine, other, which, at):
    return jnp.concatenate([mine[at, which], other[at, which]], axis=1)


def hidden_body(*refs):
    tok, cot, (w_mine, w_other) = refs[:5], refs[5:10], refs[10:12]
    act_ref, dpre_ref, given_ref, kept_ref, pre_ref, dact_ref = refs[12:]
    first = True
    for ky in range(N):
        for rc in range(2):
            at = feature_block(ky, rc)
            a = dot(rows_of(token_block, tok, ky, rc), weight_block(w_mine, w_other, 0, at), 1, 0)
            b = dot(rows_of(cotan_block, cot, ky, rc), weight_block(w_mine, w_other, 1, at), 1, 0)
            if first:
                pre_ref[...] = a
                dact_ref[...] = b
            else:
                pre_ref[...] += a
                dact_ref[...] += b
            first = False
    relued = jnp.maximum(pre_ref[...], 0.0)
    act_ref[...] = (relued * relued).astype(BF16)
    dpre_ref[...] = (dact_ref[...] * 2.0 * relued).astype(BF16)
    part = act_ref.shape[1] // 2
    for ky in range(N):
        for rc in range(2):
            at = feature_block(ky, rc)
            for which, block, held, right in (
                (0, token_block, tok, dpre_ref),
                (1, cotan_block, cot, act_ref),
            ):
                g = dot(rows_of(block, held, ky, rc), right[...], 0, 0).astype(BF16)
                kept_ref[at, which] = g[:, :part]
                given_ref[at, which] = g[:, part:]


def back_body(dpre_ref, w_mine, w_other, *outs):
    rows = dpre_ref.shape[0] // N
    for ky in range(N):
        y = lax.rem(lax.axis_index("y") + ky, N)
        for core in range(2):
            o = dot(dpre_ref[...], weight_block(w_mine, w_other, 0, 2 * y + core), 1, 1).astype(BF16)
            for kx in range(N):
                piece = o[kx * rows : (kx + 1) * rows]
                if core == 0:
                    outs[kx][ky] = piece
                else:
                    outs[N + ky][kx] = piece


def sum_pieces_body(*refs):
    ins, outs = refs[:8], refs[8:]
    for s in range(2):
        for k in range(N):
            total = sum(ins[N * s + j][k].astype(F32) for j in range(N))
            outs[N * s + k][...] = total.astype(BF16)


def last_sum_body(*refs):
    ins, kept_ref, given_ref = refs[:8], refs[8], refs[9]
    sums = [sum(ins[N * s + j][...].astype(F32) for j in range(N)) for s in range(2)]
    mine = lax.axis_index("c") == 0
    kept_ref[...] = jnp.where(mine, sums[0], sums[1]).astype(BF16)
    given_ref[...] = jnp.where(mine, sums[1], sums[0]).astype(BF16)


def add_cores_body(kept_ref, got_ref, o_ref):
    nz, nx, _, rows, _ = o_ref.shape
    for z in range(nz):
        for which in range(2):
            s = (kept_ref[z, which].astype(F32) + got_ref[z, which].astype(F32)).astype(BF16)
            for x in range(nx):
                o_ref[z, x, which] = s[x * rows : (x + 1) * rows]


def grads_body(in_ref, up_ref, down_ref, up_sq, down_sq):
    nz, nx, _, rows, part = in_ref.shape
    lanes = jnp.zeros((rows, part), F32)
    for x in range(nx):
        at = pl.ds(x * part, part)
        u = sum(in_ref[z, x, 0].astype(F32) for z in range(nz))
        d = sum(in_ref[z, x, 1].astype(F32) for z in range(nz))
        up_ref[:, at] = u
        down_ref[:, at] = d
        lanes = lanes + u * u
        down_sq[:, at] = jnp.broadcast_to(jnp.sum(d * d, axis=0, keepdims=True), (8, part))
    up_sq[...] = jnp.broadcast_to(jnp.sum(lanes.T, axis=0, keepdims=True), (8, rows))


def ring_of_four(x, swapped, axis):
    before, after = shift(x, axis, 1), shift(swapped, axis, -1)
    half = x.shape[0] // 2
    return x, after, before, shift(before[:half], axis, 1), shift(after[:half], axis, -1)


def on_device(tokens, grad_out, up_weight, down_weight):
    rows, feats = tokens.shape
    nz, nx = lax.axis_size("z"), lax.axis_size("x")
    half = rows // 2
    d_rows, hid = up_weight.shape
    part = hid // nx
    c = lax.axis_index("c")

    w = jnp.stack([up_weight, down_weight.T]).reshape(2, d_rows, nx, part)
    w = exchange(w.transpose(2, 0, 1, 3), "x")
    w = w.transpose(1, 0, 2, 3).reshape(1, 2, nx * d_rows, part)
    w_mine = exchange(jnp.broadcast_to(w, (nz, *w.shape[1:])), "z")
    w_other = shift(w_mine, "c", 1)

    both = jnp.stack([tokens, grad_out]).reshape(2, 2, half, feats)
    keep = lax.dynamic_index_in_dim(both, c, 1, keepdims=False)
    give = lax.dynamic_index_in_dim(both, 1 - c, 1, keepdims=False)
    got = shift(give, "c", 1)

    def near(k, axis):
        block = jnp.stack([keep[k], got[k]])
        around = [block] + [shift(block, axis, -s) for s in range(1, N)]
        return jnp.stack(around), jnp.stack(around[2:] + around[:2])

    tok = ring_of_four(*near(0, "x"), "y")
    cot = ring_of_four(*near(1, "y"), "x")

    nrows, width = N * half, 2 * part
    one = 2 * nrows * 2 * N * feats * width
    act, dpre, given, kept = pl.pallas_call(
        hidden_body,
        out_shape=[
            out(BF16, nrows, width),
            out(BF16, nrows, width),
            out(BF16, nz, 2, feats, part),
            out(BF16, nz, 2, feats, part),
        ],
        in_specs=[VMEM] * 12,
        out_specs=[VMEM] * 4,
        scratch_shapes=[pltpu.VMEM((nrows, width), F32), pltpu.VMEM((nrows, width), F32)],
        cost_estimate=pl.CostEstimate(flops=4 * one, bytes_accessed=2**23, transcendentals=0),
        compiler_params=pltpu.CompilerParams(vmem_limit_bytes=48 * 2**20),
        name="hidden",
    )(*tok, *cot, w_mine, w_other)

    arrived = shift(given, "c", 1)
    (sent,) = kernel(add_cores_body, [out(BF16, nz, nx, 2, d_rows, part)], (kept, arrived), 10**6, "add_cores")
    summed = exchange(sent.reshape(nz * nx, 2, d_rows, part), ("z", "x"))

    pieces = kernel(back_body, [out(BF16, N, half, feats)] * 8, (dpre, w_mine, w_other), one, "back")
    first = [shift(pieces[k], "x", k) if k else pieces[0] for k in range(N)]
    first += [shift(pieces[N + k], "y", k) if k else pieces[N] for k in range(N)]
    pieces = kernel(sum_pieces_body, [out(BF16, half, feats)] * 8, first, 10**6, "sum_pieces")
    second = [shift(pieces[k], "y", k) if k else pieces[0] for k in range(N)]
    second += [shift(pieces[N + k], "x", k) if k else pieces[N] for k in range(N)]
    ours, theirs = kernel(last_sum_body, [out(BF16, half, feats)] * 2, second, 10**6, "last_sum")
    theirs = shift(theirs, "c", 1)
    input_grad = jnp.where(
        c == 0, jnp.concatenate([ours, theirs]), jnp.concatenate([theirs, ours])
    )

    up_grad, down_flip, up_sq, down_sq = kernel(
        grads_body,
        [out(F32, d_rows, hid), out(F32, d_rows, hid), out(F32, 8, d_rows), out(F32, 8, hid)],
        (summed.reshape(nz, nx, 2, d_rows, part),),
        10**6,
        "grads",
    )
    up_sq, down_sq = up_sq[:1], down_sq[:1]
    down_norms = exchange(jnp.broadcast_to(down_sq, (nz * nx, 1, hid)), ("z", "x")).sum(axis=(0, 1))
    up_sq = up_sq + shift(up_sq, "c", 1)
    up_norms = sum([up_sq] + [shift(up_sq, "y", s) for s in range(1, N)])[0]
    return input_grad, up_grad, down_flip.T, up_norms, down_norms


def solution(mesh):
    finer = Mesh(mesh.devices.reshape(8, 4, 4, 2), ("z", "x", "y", "c"))
    fs, tp = ("z", "x"), ("y", "c")
    return jax.shard_map(
        on_device,
        mesh=finer,
        in_specs=(P(fs, tp), P(fs, tp), P(fs, tp), P(tp, fs)),
        out_specs=(P(fs, tp), P(fs, tp), P(tp, fs), P(fs), P(tp)),
        check_vma=False,
    )
```
